32 devices in a mesh: sp: 8 (over z, x), dp: 4 (over y, core).
Axes of the slice: x: 2, y: 2, z: 4, core: 2. Of those that a mesh axis runs over, the one named last changes fastest.
Arguments:
- tokens: bfloat16 [32, 512, 2048], P('dp', 'sp'), may hold values from -6 to 6
- pre_gain: float32 [2048], replicated, may hold values from 0.1 to 1.9
- w_query: bfloat16 [2048, 512], P('dp'), may hold values from -0.125 to 0.125
- w_forget: bfloat16 [2048, 512], P('dp'), may hold values from -0.125 to 0.125
- w_value: bfloat16 [2048, 512], P('dp'), may hold values from -0.125 to 0.125
- w_gate: bfloat16 [2048, 512], P('dp'), may hold values from -0.125 to 0.125
- lower_bound: float32 [512], replicated, may hold values from 0.8 to 1
- extra_decay: float32 [128, 512], P(('dp', 'sp')), may hold values from -1.5 to 0
- initial_state: float32 [128, 128, 128], P(('dp', 'sp')), may hold values from -0.18 to 0.18
- norm_gain: float32 [128], replicated, may hold values from 0.1 to 1.9
- w_out: bfloat16 [512, 2048], P('dp'), may hold values from -0.25 to 0.25
- post_gain: float32 [2048], replicated, may hold values from 0.1 to 1.9
Outputs:
- layer_out: bfloat16 [32, 512, 2048], P('dp', 'sp')
The draws below stay inside these ranges and needn't reach their ends.
All inputs are finite; a program needn't handle non-finite values.
Results may differ from the reference program's by a relative error of at most 0.015.
Values may be sent and summed in bfloat16 or wider, within the bound.
A program may use at most 64 MiB of HBM per device.

```python
import math
import jax
import jax.numpy as jnp
from jax import lax

D = 2048
HEADS = 4
HK = 128
HV = 128
BLOCK = 64
LOC = 64
SEQUENCE_LENGTH = 512
SEQS = 32


def draw_lower_bound(key, part):
    key_rows = jax.random.split(jax.random.fold_in(key, 11), 4)
    order = jax.random.permutation(key_rows[0], HEADS)
    fast_count = HEADS // 2
    fast_heads = order < fast_count
    slow_gap = jax.random.uniform(key_rows[1], (HEADS, 1), jnp.float32, 0.1, 0.5) / SEQUENCE_LENGTH
    fast_gap = jnp.exp(jax.random.uniform(key_rows[2], (HEADS, 1), jnp.float32, math.log(1.0 / 40.0), math.log(1.0 / 15.0)))
    spread = jnp.exp(jax.random.uniform(key_rows[3], (HEADS, HK), jnp.float32, math.log(0.5), math.log(2.0)))
    forget_gap = jnp.where(fast_heads[:, None], fast_gap, slow_gap) * spread
    return (1.0 - forget_gap).reshape(HEADS * HK)


def draw_extra_decay(key, part):
    key_rows = jax.random.split(jax.random.fold_in(key, 23), 3)
    count_of_rows = SEQS * HEADS
    block_count = SEQUENCE_LENGTH // LOC
    rate_low = 0.3
    rates = jnp.exp(jax.random.uniform(key_rows[0], (count_of_rows, block_count), jnp.float32, math.log(rate_low), math.log(1.2))) / SEQUENCE_LENGTH
    base_offset = -jnp.repeat(rates, LOC, axis=1)
    spike_position = jax.random.randint(key_rows[1], (count_of_rows, 2), 0, SEQUENCE_LENGTH)
    spike_fraction = jax.random.uniform(key_rows[2], (count_of_rows, 2), jnp.float32, 0.2, 0.5)
    token_position = jnp.arange(SEQUENCE_LENGTH, dtype=jnp.int32)
    match_count = token_position[None, None, :] == spike_position[:, :, None]
    spike_events = jnp.sum(jnp.where(match_count, jnp.log1p(-spike_fraction)[:, :, None], 0.0), axis=1)
    return base_offset + spike_events


def block_levels(own_key, extent, cuts, low, largest):
    factor_of, own = 1.0, jax.random.fold_in(own_key, 6)
    for position, parts in cuts:
        draws = jnp.exp(jax.random.uniform(jax.random.fold_in(own, position), (parts,), jnp.float32, low / len(cuts), largest / len(cuts)))
        factor_of = factor_of * jnp.repeat(draws, extent[position] // parts).reshape([-1 if axis == position else 1 for axis in range(len(extent))])
    return factor_of


def scatter_about(key, dims, width, bound, cuts=(), held_as=jnp.bfloat16):
    level = block_levels(key, dims, cuts, -0.22, 0.18) if cuts else 1.0
    entries = jax.random.normal(key, dims, jnp.float32) * width * level
    return jnp.minimum(jnp.maximum(entries, -bound), bound).astype(held_as)


def setup_inputs(seed: int = 0) -> dict:
    key_of = jax.random.split(jax.random.key(seed), 13)
    return {
        "tokens": scatter_about(key_of[0], (SEQS, SEQUENCE_LENGTH, D), 1.0, 6.0, ((0, 4), (1, 8))),
        "pre_gain": jnp.clip(1.0 + 0.18 * jax.random.normal(key_of[1], (D,), jnp.float32), 0.1, 1.9),
        "w_query": scatter_about(key_of[2], (D, HEADS * HK), D ** -0.5, 0.125, ((0, 4),)),
        "w_forget": scatter_about(key_of[3], (D, HEADS * HK), D ** -0.5, 0.125, ((0, 4),)),
        "w_value": scatter_about(key_of[4], (D, HEADS * HV), D ** -0.5, 0.125, ((0, 4),)),
        "w_gate": scatter_about(key_of[5], (D, HEADS * HV), D ** -0.5, 0.125, ((0, 4),)),
        "lower_bound": draw_lower_bound(jax.random.fold_in(key_of[12], 71), 0),
        "extra_decay": draw_extra_decay(jax.random.fold_in(key_of[12], 71), 0),
        "initial_state": scatter_about(key_of[8], (SEQS * HEADS, HK, HV), 0.03, 0.18, ((0, 32),), jnp.float32),
        "norm_gain": jnp.clip(1.0 + 0.18 * jax.random.normal(key_of[9], (HV,), jnp.float32), 0.1, 1.9),
        "w_out": scatter_about(key_of[10], (HEADS * HV, D), (HEADS * HV) ** -0.5, 0.25, ((0, 4),)),
        "post_gain": jnp.clip(1.0 + 0.18 * jax.random.normal(key_of[11], (D,), jnp.float32), 0.1, 1.9),
    }


EPS = 1e-06

def rms_scale(matrix, gain):
    widened = matrix.astype(jnp.float32)
    return widened * lax.rsqrt(lax.optimization_barrier(jnp.mean(widened * widened, axis=-1, keepdims=True)) + EPS) * gain

def recur_item(queries, keys_in, values, log_decay, state_zero):
    length = queries.shape[0]
    block_count = length // BLOCK

    def blocks(matrix):
        return matrix.reshape(block_count, BLOCK, matrix.shape[-1])
    causal_mask = jnp.tril(jnp.ones((BLOCK, BLOCK), dtype=bool))[:, :, None]

    def block_step(carried_state, inputs):
        query_block, key_block, value_block, decay_block = inputs
        cumulative = jnp.cumsum(decay_block, axis=0)
        carried = jnp.dot(query_block * jnp.exp(cumulative), carried_state, precision=lax.Precision.HIGHEST)
        log_gaps = cumulative[:, None, :] - cumulative[None, :, :]
        decay_weight = jnp.where(causal_mask, jnp.exp(jnp.minimum(log_gaps, 0.0)), 0.0)
        scores = jnp.einsum('tk,sk,tsk->ts', query_block, key_block, decay_weight, precision=lax.Precision.HIGHEST)
        within = jnp.dot(scores, value_block, precision=lax.Precision.HIGHEST)
        block_end = cumulative[-1]
        added_state = jnp.dot((key_block * jnp.exp(block_end[None, :] - cumulative)).T, value_block, precision=lax.Precision.HIGHEST)
        return (jnp.exp(block_end)[:, None] * carried_state + added_state, carried + within)
    _, block_outs = lax.scan(block_step, state_zero, (blocks(queries), blocks(keys_in), blocks(values), blocks(log_decay)))
    return block_outs.reshape(length, values.shape[-1])

def reference(tokens, pre_gain, w_query, w_forget, w_value, w_gate, lower_bound, extra_decay, initial_state, norm_gain, w_out, post_gain):
    forget_gap = (1.0 - lower_bound).reshape(HEADS, HK)
    states = initial_state.reshape(SEQS, HEADS, HK, HV)
    extras = extra_decay.reshape(SEQS, HEADS, SEQUENCE_LENGTH)
    query_weight = w_query.reshape(D, HEADS, HK).astype(jnp.float32)
    forget_weight = w_forget.reshape(D, HEADS, HK).astype(jnp.float32)
    value_weight = w_value.reshape(D, HEADS, HV).astype(jnp.float32)
    gate_weight = w_gate.reshape(D, HEADS, HV).astype(jnp.float32)
    out_weight = w_out.reshape(HEADS, HV, D).astype(jnp.float32)

    def one_sequence(inputs):
        row_block, state_zero, extra_rows = inputs
        norm_result = rms_scale(row_block, pre_gain).astype(jnp.bfloat16).astype(jnp.float32)
        q_pre = jnp.einsum('ld,dhk->hlk', norm_result, query_weight).astype(jnp.bfloat16)
        f_pre = jnp.einsum('ld,dhk->hlk', norm_result, forget_weight).astype(jnp.bfloat16)
        v_pre = jnp.einsum('ld,dhk->hlk', norm_result, value_weight).astype(jnp.bfloat16)
        g_pre = jnp.einsum('ld,dhk->hlk', norm_result, gate_weight).astype(jnp.bfloat16)
        queries = jax.nn.silu(q_pre.astype(jnp.float32))
        keys_in = forget_gap[:, None, :] * jax.nn.sigmoid(-f_pre.astype(jnp.float32))
        log_decay = jnp.log1p(-keys_in) + extra_rows[:, :, None]
        values = v_pre.astype(jnp.float32)
        outputs = jax.vmap(recur_item)(queries, keys_in, values, log_decay, state_zero)
        head_normed = (outputs * lax.rsqrt(lax.optimization_barrier(jnp.mean(outputs * outputs, axis=-1, keepdims=True)) + EPS) * norm_gain).astype(jnp.bfloat16)
        head_normed = lax.optimization_barrier(head_normed)
        gated = (head_normed.astype(jnp.float32) * jax.nn.silu(g_pre.astype(jnp.float32))).astype(jnp.bfloat16)
        mixed = jnp.einsum('hlv,hvd->ld', gated.astype(jnp.float32), out_weight)
        return rms_scale(mixed, post_gain).astype(jnp.bfloat16)
    return lax.map(one_sequence, (tokens, states, extras))
```

```python
import functools

import jax
import jax.numpy as jnp
from jax import lax
from jax.experimental import pallas as pl
from jax.experimental.pallas import tpu as pltpu
from jax.sharding import PartitionSpec as P

EPS = 1e-06
MESH = pl.DeviceIdType.MESH


def rms_scale(matrix, gain):
    widened = matrix.astype(jnp.float32)
    return widened * lax.rsqrt(jnp.mean(widened * widened, axis=-1, keepdims=True) + EPS) * gain


def gather_rows(pieces):
    ways = lax.axis_size("sp")
    share = pieces.shape[0] // ways
    mine = lax.dynamic_slice_in_dim(pieces, lax.axis_index("sp") * share, share, axis=0)
    return lax.all_gather(mine, ("dp", "sp"), axis=0, tiled=True)


def chain_kernel(
    n,
    heads,
    f_v_ref,
    q_g_ref,
    extra_ref,
    gap_ref,
    init_ref,
    gain_ref,
    out_ref,
    rbuf,
    sbuf,
    send_sem,
    recv_sem,
    init_sem,
):
    me = lax.axis_index("sp")
    items, hv, hk = rbuf.shape
    own = init_ref.shape[0]
    length = extra_ref.shape[1]
    seqs = items // heads
    cols = heads * hk

    barrier = pltpu.get_barrier_semaphore()
    for offset in range(1, n):
        pl.semaphore_signal(
            barrier, inc=1, device_id={"sp": lax.rem(me + offset, n)}, device_id_type=MESH
        )
    pl.semaphore_wait(barrier, n - 1)

    def init_copy(j):
        return pltpu.make_async_remote_copy(
            src_ref=init_ref.at[j],
            dst_ref=rbuf.at[me * own + j],
            send_sem=init_sem.at[j],
            recv_sem=recv_sem.at[me * own + j],
            device_id={"sp": 0},
            device_id_type=MESH,
        )

    def chain_copy(it):
        return pltpu.make_async_remote_copy(
            src_ref=sbuf.at[it],
            dst_ref=rbuf.at[it],
            send_sem=send_sem.at[it],
            recv_sem=recv_sem.at[it],
            device_id={"sp": lax.rem(me + 1, n)},
            device_id_type=MESH,
        )

    @pl.when(me > 0)
    def _():
        for j in range(own):
            init_copy(j).start()

    @pl.when(me == 0)
    def _():
        rbuf[0:own] = init_ref[...]

    row = lax.broadcasted_iota(jnp.int32, (length, length), 0)
    col = lax.broadcasted_iota(jnp.int32, (length, length), 1)
    causal = row >= col
    ones = causal.astype(jnp.float32)
    nt = (((1,), (1,)), ((), ()))
    tn = (((0,), (0,)), ((), ()))

    def sequence(s, carry):
        rows = pl.ds(pl.multiple_of(s * length, length), length)
        f_pre = f_v_ref[rows, 0:cols].astype(jnp.float32)
        keys = gap_ref[...] * jax.nn.sigmoid(-f_pre)
        extra = extra_ref[s]
        spread = jnp.concatenate(
            [jnp.broadcast_to(extra[:, h : h + 1], (length, hk)) for h in range(heads)], axis=1
        )
        decay = jnp.log1p(-keys) + spread
        cum = jnp.dot(
            ones, decay, precision=lax.Precision.HIGHEST, preferred_element_type=jnp.float32
        )
        end = cum[length - 1 : length, :]
        mid = cum[length // 2 : length // 2 + 1, :]
        keys_end = (keys * jnp.exp(end - cum)).astype(jnp.bfloat16)
        keys_mid = (keys * jnp.exp(mid - cum)).astype(jnp.bfloat16)
        end_decay = jnp.exp(end)
        q_pre = q_g_ref[rows, 0:cols].astype(jnp.float32)
        queries = q_pre * jax.nn.sigmoid(q_pre)
        q_carry = (queries * jnp.exp(cum)).astype(jnp.bfloat16)
        q_mid = (queries * jnp.exp(cum - mid)).astype(jnp.bfloat16)
        within = []
        added = []
        for h in range(heads):
            lanes = slice(h * hk, (h + 1) * hk)
            values = f_v_ref[rows, cols + h * hv : cols + (h + 1) * hv]
            added.append(
                lax.dot_general(
                    values, keys_end[:, lanes], tn, preferred_element_type=jnp.float32
                )
            )
            scores = lax.dot_general(
                q_mid[:, lanes], keys_mid[:, lanes], nt, preferred_element_type=jnp.float32
            )
            scores = jnp.where(causal, scores, 0.0).astype(jnp.bfloat16)
            within.append(jnp.dot(scores, values, preferred_element_type=jnp.float32))
        for h in range(heads):
            lanes = slice(h * hk, (h + 1) * hk)
            it = s * heads + h

            @pl.when(jnp.logical_or(me > 0, it >= own))
            def _():
                chain_copy(it).wait_recv()

            @pl.when(me < n - 1)
            def _():
                state = rbuf[it].astype(jnp.float32)
                sbuf[it] = (state * end_decay[:, lanes] + added[h]).astype(jnp.bfloat16)
                chain_copy(it).start()

        for h in range(heads):
            lanes = slice(h * hk, (h + 1) * hk)
            it = s * heads + h
            outs = within[h] + lax.dot_general(
                q_carry[:, lanes], rbuf[it], nt, preferred_element_type=jnp.float32
            )
            normed = rms_scale(outs, gain_ref[...]).astype(jnp.bfloat16).astype(jnp.float32)
            g_pre = q_g_ref[rows, cols + h * hv : cols + (h + 1) * hv].astype(jnp.float32)
            out_ref[rows, h * hv : (h + 1) * hv] = (
                normed * (g_pre * jax.nn.sigmoid(g_pre))
            ).astype(jnp.bfloat16)
        return carry

    lax.fori_loop(0, seqs, sequence, 0)

    @pl.when(me > 0)
    def _():
        for j in range(own):
            init_copy(j).wait_send()

    @pl.when(me < n - 1)
    def _():
        def done(it, carry):
            chain_copy(it).wait_send()
            return carry

        lax.fori_loop(0, items, done, 0)


def recurrence(f_v, q_g, extra, gap, init, gain, heads, n):
    own, hv, hk = init.shape
    items = own * n
    vmem = pl.BlockSpec(memory_space=pltpu.VMEM)
    return pl.pallas_call(
        functools.partial(chain_kernel, n, heads),
        out_shape=jax.ShapeDtypeStruct((f_v.shape[0], heads * hv), jnp.bfloat16),
        in_specs=[vmem] * 6,
        out_specs=vmem,
        scratch_shapes=[
            pltpu.VMEM((items, hv, hk), jnp.bfloat16),
            pltpu.VMEM((items, hv, hk), jnp.bfloat16),
            pltpu.SemaphoreType.DMA((items,)),
            pltpu.SemaphoreType.DMA((items,)),
            pltpu.SemaphoreType.DMA((own,)),
        ],
        compiler_params=pltpu.CompilerParams(
            collective_id=0, has_side_effects=True, vmem_limit_bytes=24 * 1024 * 1024
        ),
        cost_estimate=pl.CostEstimate(flops=10**9, bytes_accessed=10**8, transcendentals=10**6),
    )(f_v, q_g, extra, gap, init, gain)


def body(
    n,
    tokens,
    pre_gain,
    w_query,
    w_forget,
    w_value,
    w_gate,
    lower_bound,
    extra_decay,
    initial_state,
    norm_gain,
    w_out,
    post_gain,
):
    seq_count, local_len, width = tokens.shape
    own, hk, hv = initial_state.shape
    heads = w_query.shape[1] // hk
    w_f_v = gather_rows(jnp.concatenate([w_forget, w_value], axis=1))
    w_q_g = gather_rows(jnp.concatenate([w_query, w_gate], axis=1))
    w_o = gather_rows(w_out)
    extra = lax.all_to_all(extra_decay, "sp", split_axis=1, concat_axis=0, tiled=True)
    extra = extra.reshape(seq_count, heads, local_len).transpose(0, 2, 1)
    init = jnp.swapaxes(initial_state, 1, 2).astype(jnp.bfloat16)
    normed = rms_scale(tokens, pre_gain).astype(jnp.bfloat16).reshape(seq_count * local_len, width)
    f_v = jnp.dot(normed, w_f_v, preferred_element_type=jnp.float32).astype(jnp.bfloat16)
    q_g = jnp.dot(normed, w_q_g, preferred_element_type=jnp.float32).astype(jnp.bfloat16)
    gated = recurrence(
        f_v, q_g, extra, (1.0 - lower_bound)[None, :], init, norm_gain[None, :], heads, n
    )
    mixed = jnp.dot(gated, w_o, preferred_element_type=jnp.float32)
    return rms_scale(mixed, post_gain).astype(jnp.bfloat16).reshape(seq_count, local_len, width)


def solution(mesh):
    in_specs = (
        P("dp", "sp", None),
        P(),
        P("dp", None),
        P("dp", None),
        P("dp", None),
        P("dp", None),
        P(),
        P(("dp", "sp"), None),
        P(("dp", "sp"), None, None),
        P(),
        P("dp", None),
        P(),
    )
    out_specs = P("dp", "sp", None)
    return jax.shard_map(
        functools.partial(body, mesh.shape["sp"]),
        mesh=mesh,
        in_specs=in_specs,
        out_specs=out_specs,
        check_vma=False,
    )
```

```python
import functools

import jax
import jax.numpy as jnp
from jax import lax
from jax.experimental import pallas as pl
from jax.experimental.pallas import tpu as pltpu
from jax.sharding import PartitionSpec as P

EPS = 1e-06
MESH = pl.DeviceIdType.MESH


def rms_scale(matrix, gain):
    widened = matrix.astype(jnp.float32)
    return widened * lax.rsqrt(jnp.mean(widened * widened, axis=-1, keepdims=True) + EPS) * gain


def layer_kernel(
    n,
    ways,
    heads,
    tokens_ref,
    pre_ref,
    w0,
    w1,
    w2,
    w3,
    w4,
    extra_ref,
    gap_ref,
    init_ref,
    gain_ref,
    out_ref,
    a4,
    a0,
    a1,
    a2,
    a3,
    normed,
    f_v_ref,
    q_g_ref,
    cum_ref,
    keys_ref,
    rbuf,
    sbuf,
    send_sem,
    recv_sem,
    init_sem,
    y_send,
    y_recv,
    x_send,
    x_recv,
    s_send,
    s_recv,
    local_sem,
):
    me = lax.axis_index("sp")
    rank = lax.axis_index("dp")
    items, hv, hk = rbuf.shape
    own = init_ref.shape[0]
    seqs, length, width = tokens_ref.shape
    cols = heads * hk
    tile = 2 * hk
    shards = (w0, w1, w2, w3, w4)
    wholes = (a0, a1, a2, a3, a4)
    side = lax.rem(me, 2)
    beside = me + 1 - 2 * side
    sibling = rank + 1 - 2 * lax.rem(rank, 2)
    peers = ways // 2 - 1

    barrier = pltpu.get_barrier_semaphore()
    for offset in range(1, n):
        pl.semaphore_signal(
            barrier, inc=1, device_id={"sp": lax.rem(me + offset, n)}, device_id_type=MESH
        )
    for offset in range(1, ways):
        pl.semaphore_signal(
            barrier, inc=1, device_id={"dp": lax.rem(rank + offset, ways)}, device_id_type=MESH
        )
    pl.semaphore_wait(barrier, n + ways - 2)

    def part(w, shard, half):
        rows = shards[w].shape[0]
        start = shard * rows + half * (rows // 2)
        return wholes[w].at[pl.ds(pl.multiple_of(start, rows // 2), rows // 2)]

    def full(w, shard):
        rows = shards[w].shape[0]
        return wholes[w].at[pl.ds(pl.multiple_of(shard * rows, rows), rows)]

    def remote(src, dst, send, recv, device):
        return pltpu.make_async_remote_copy(
            src_ref=src,
            dst_ref=dst,
            send_sem=send,
            recv_sem=recv,
            device_id=device,
            device_id_type=MESH,
        )

    def y_copy(w, k):
        rows = shards[w].shape[0] // 2
        src = shards[w].at[pl.ds(pl.multiple_of(side * rows, rows), rows)]
        target = lax.rem(rank + 2 * (k + 1), ways)
        return remote(src, part(w, rank, side), y_send.at[w, k], y_recv.at[w, k], {"dp": target})

    def origin(k):
        return lax.rem(rank + ways - 2 * (k + 1), ways)

    def x_copy(w, k):
        ref = part(w, origin(k), side)
        return remote(ref, ref, x_send.at[w, k], x_recv.at[w, k], {"sp": beside})

    def s_own(w):
        return remote(
            shards[w], full(w, rank), s_send.at[w, 0], s_recv.at[w, 0], {"dp": sibling}
        )

    def s_copy(w, k, second):
        ref = part(w, origin(k), 1 - side if second else side)
        slot = 1 + 2 * k + second
        return remote(ref, ref, s_send.at[w, slot], s_recv.at[w, slot], {"dp": sibling})

    def local_copy(w):
        return pltpu.make_async_copy(shards[w], full(w, rank), local_sem.at[w])

    def pass_y(w):
        for k in range(peers):
            y_copy(w, k).wait_recv()
            x_copy(w, k).start()
            s_copy(w, k, 0).start()

    def pass_x(w):
        for k in range(peers):
            x_copy(w, k).wait_recv()
            s_copy(w, k, 1).start()

    def arrived(w):
        s_own(w).wait_recv()
        for k in range(peers):
            s_copy(w, k, 0).wait_recv()
            s_copy(w, k, 1).wait_recv()

    def init_copy(j):
        return remote(
            init_ref.at[j],
            rbuf.at[me * own + j],
            init_sem.at[j],
            recv_sem.at[me * own + j],
            {"sp": 0},
        )

    def chain_copy(it):
        return remote(
            sbuf.at[it],
            rbuf.at[it],
            send_sem.at[it],
            recv_sem.at[it],
            {"sp": lax.rem(me + 1, n)},
        )

    for w in range(5):
        for k in range(peers):
            y_copy(w, k).start()
        s_own(w).start()
        local_copy(w).start()

    @pl.when(me > 0)
    def _():
        for j in range(own):
            init_copy(j).start()

    @pl.when(me == 0)
    def _():
        rbuf[0:own] = init_ref[...]

    def norm_rows(s, carry):
        rows = pl.ds(pl.multiple_of(s * length, length), length)
        normed[rows, :] = rms_scale(tokens_ref[s], pre_ref[...]).astype(jnp.bfloat16)
        return carry

    lax.fori_loop(0, seqs, norm_rows, 0)

    def project(w, dest, at, j):
        lanes = pl.ds(pl.multiple_of(j * tile, tile), tile)
        where = pl.ds(pl.multiple_of(at + j * tile, tile), tile)
        dest[:, where] = jnp.dot(
            normed[...], wholes[w][:, lanes], preferred_element_type=jnp.float32
        ).astype(jnp.bfloat16)

    def project_all(w, dest, at):
        def step(j, carry):
            project(w, dest, at, j)
            return carry

        lax.fori_loop(0, cols // tile, step, 0)

    for w in range(5):
        local_copy(w).wait()
    pass_y(0)
    pass_y(1)
    pass_x(0)
    arrived(0)
    project_all(0, f_v_ref, 0)
    pass_x(1)
    pass_y(2)
    arrived(1)
    project_all(1, f_v_ref, cols)
    pass_x(2)
    pass_y(3)
    pass_x(3)
    pass_y(4)

    row = lax.broadcasted_iota(jnp.int32, (length, length), 0)
    col = lax.broadcasted_iota(jnp.int32, (length, length), 1)
    causal = row >= col
    ones = causal.astype(jnp.float32)
    nt = (((1,), (1,)), ((), ()))
    tn = (((0,), (0,)), ((), ()))
    tiles = cols // tile

    def forward(s, carry):
        rows = pl.ds(pl.multiple_of(s * length, length), length)
        f_pre = f_v_ref[rows, 0:cols].astype(jnp.float32)
        keys = gap_ref[...] * jax.nn.sigmoid(-f_pre)
        extra = extra_ref[s]
        spread = jnp.concatenate(
            [jnp.broadcast_to(extra[:, h : h + 1], (length, hk)) for h in range(heads)], axis=1
        )
        decay = jnp.log1p(-keys) + spread
        cum = jnp.dot(
            ones, decay, precision=lax.Precision.HIGHEST, preferred_element_type=jnp.float32
        )
        end = cum[length - 1 : length, :]
        mid = cum[length // 2 : length // 2 + 1, :]
        keys_end = (keys * jnp.exp(end - cum)).astype(jnp.bfloat16)
        keys_ref[rows, :] = (keys * jnp.exp(mid - cum)).astype(jnp.bfloat16)
        cum_ref[rows, :] = cum
        end_decay = jnp.exp(end)
        added = []
        for h in range(heads):
            lanes = slice(h * hk, (h + 1) * hk)
            values = f_v_ref[rows, cols + h * hv : cols + (h + 1) * hv]
            added.append(
                lax.dot_general(
                    values, keys_end[:, lanes], tn, preferred_element_type=jnp.float32
                )
            )
        for h in range(heads):
            lanes = slice(h * hk, (h + 1) * hk)
            it = s * heads + h

            @pl.when(jnp.logical_or(me > 0, it >= own))
            def _():
                chain_copy(it).wait_recv()

            @pl.when(me < n - 1)
            def _():
                state = rbuf[it].astype(jnp.float32)
                sbuf[it] = (state * end_decay[:, lanes] + added[h]).astype(jnp.bfloat16)
                chain_copy(it).start()

        @pl.when(s == 0)
        def _():
            arrived(2)

        @pl.when(s == tiles)
        def _():
            arrived(3)

        @pl.when(s < tiles)
        def _():
            project(2, q_g_ref, 0, s)

        @pl.when(jnp.logical_and(s >= tiles, s < 2 * tiles))
        def _():
            project(3, q_g_ref, cols, s - tiles)

        return carry

    lax.fori_loop(0, seqs, forward, 0)
    pass_x(4)

    def outputs(s, carry):
        rows = pl.ds(pl.multiple_of(s * length, length), length)
        cum = cum_ref[rows, :]
        mid = cum[length // 2 : length // 2 + 1, :]
        q_pre = q_g_ref[rows, 0:cols].astype(jnp.float32)
        queries = q_pre * jax.nn.sigmoid(q_pre)
        q_carry = (queries * jnp.exp(cum)).astype(jnp.bfloat16)
        q_mid = (queries * jnp.exp(cum - mid)).astype(jnp.bfloat16)
        for h in range(heads):
            lanes = slice(h * hk, (h + 1) * hk)
            it = s * heads + h
            values = f_v_ref[rows, cols + h * hv : cols + (h + 1) * hv]
            scores = lax.dot_general(
                q_mid[:, lanes], keys_ref[rows, lanes], nt, preferred_element_type=jnp.float32
            )
            scores = jnp.where(causal, scores, 0.0).astype(jnp.bfloat16)
            outs = jnp.dot(scores, values, preferred_element_type=jnp.float32) + lax.dot_general(
                q_carry[:, lanes], rbuf[it], nt, preferred_element_type=jnp.float32
            )
            scaled = rms_scale(outs, gain_ref[...]).astype(jnp.bfloat16).astype(jnp.float32)
            g_pre = q_g_ref[rows, cols + h * hv : cols + (h + 1) * hv].astype(jnp.float32)
            out_ref[rows, h * hv : (h + 1) * hv] = (
                scaled * (g_pre * jax.nn.sigmoid(g_pre))
            ).astype(jnp.bfloat16)
        return carry

    lax.fori_loop(0, seqs, outputs, 0)
    arrived(4)
    for w in range(5):
        s_own(w).wait_send()
        for k in range(peers):
            y_copy(w, k).wait_send()
            x_copy(w, k).wait_send()
            s_copy(w, k, 0).wait_send()
            s_copy(w, k, 1).wait_send()

    @pl.when(me > 0)
    def _():
        for j in range(own):
            init_copy(j).wait_send()

    @pl.when(me < n - 1)
    def _():
        def done(it, carry):
            chain_copy(it).wait_send()
            return carry

        lax.fori_loop(0, items, done, 0)


def layer(tokens, pre, weights, extra, gap, init, gain, n, ways):
    own, hv, hk = init.shape
    seqs, length, width = tokens.shape
    items = own * n
    heads = items // seqs
    rows = seqs * length
    peers = max(ways // 2 - 1, 1)
    vmem = pl.BlockSpec(memory_space=pltpu.VMEM)
    dma = pltpu.SemaphoreType.DMA

    def whole(w):
        return (w.shape[0] * ways, w.shape[1])

    return pl.pallas_call(
        functools.partial(layer_kernel, n, ways, heads),
        out_shape=[
            jax.ShapeDtypeStruct((rows, heads * hv), jnp.bfloat16),
            jax.ShapeDtypeStruct(whole(weights[4]), jnp.bfloat16),
        ],
        in_specs=[vmem] * 11,
        out_specs=[vmem] * 2,
        scratch_shapes=[pltpu.VMEM(whole(w), jnp.bfloat16) for w in weights[:4]]
        + [
            pltpu.VMEM((rows, width), jnp.bfloat16),
            pltpu.VMEM((rows, heads * (hk + hv)), jnp.bfloat16),
            pltpu.VMEM((rows, heads * (hk + hv)), jnp.bfloat16),
            pltpu.VMEM((rows, heads * hk), jnp.float32),
            pltpu.VMEM((rows, heads * hk), jnp.bfloat16),
            pltpu.VMEM((items, hv, hk), jnp.bfloat16),
            pltpu.VMEM((items, hv, hk), jnp.bfloat16),
            dma((items,)),
            dma((items,)),
            dma((own,)),
            dma((5, peers)),
            dma((5, peers)),
            dma((5, peers)),
            dma((5, peers)),
            dma((5, 1 + 2 * peers)),
            dma((5, 1 + 2 * peers)),
            dma((5,)),
        ],
        compiler_params=pltpu.CompilerParams(
            collective_id=0, has_side_effects=True, vmem_limit_bytes=48 * 1024 * 1024
        ),
        cost_estimate=pl.CostEstimate(
            flops=6 * 10**9, bytes_accessed=2 * 10**7, transcendentals=10**6
        ),
    )(tokens, pre, *weights, extra, gap, init, gain)


def body(
    n,
    ways,
    tokens,
    pre_gain,
    w_query,
    w_forget,
    w_value,
    w_gate,
    lower_bound,
    extra_decay,
    initial_state,
    norm_gain,
    w_out,
    post_gain,
):
    seq_count, local_len, width = tokens.shape
    heads = w_query.shape[1] // initial_state.shape[1]
    extra = lax.all_to_all(extra_decay, "sp", split_axis=1, concat_axis=0, tiled=True)
    extra = extra.reshape(seq_count, heads, local_len).transpose(0, 2, 1)
    init = jnp.swapaxes(initial_state, 1, 2).astype(jnp.bfloat16)
    gated, w_o = layer(
        tokens,
        pre_gain[None, :],
        (w_forget, w_value, w_query, w_gate, w_out),
        extra,
        (1.0 - lower_bound)[None, :],
        init,
        norm_gain[None, :],
        n,
        ways,
    )
    mixed = jnp.dot(gated, w_o, preferred_element_type=jnp.float32)
    return rms_scale(mixed, post_gain).astype(jnp.bfloat16).reshape(seq_count, local_len, width)


def solution(mesh):
    in_specs = (
        P("dp", "sp", None),
        P(),
        P("dp", None),
        P("dp", None),
        P("dp", None),
        P("dp", None),
        P(),
        P(("dp", "sp"), None),
        P(("dp", "sp"), None, None),
        P(),
        P("dp", None),
        P(),
    )
    out_specs = P("dp", "sp", None)
    return jax.shard_map(
        functools.partial(body, mesh.shape["sp"], mesh.shape["dp"]),
        mesh=mesh,
        in_specs=in_specs,
        out_specs=out_specs,
        check_vma=False,
    )
```

```python
import functools

import jax
import jax.numpy as jnp
from jax import lax
from jax.experimental import pallas as pl
from jax.experimental.pallas import tpu as pltpu
from jax.sharding import PartitionSpec as P

EPS = 1e-06
MESH = pl.DeviceIdType.MESH


def rms_scale(matrix, gain):
    widened = matrix.astype(jnp.float32)
    return widened * lax.rsqrt(jnp.mean(widened * widened, axis=-1, keepdims=True) + EPS) * gain


def layer_kernel(
    n,
    ways,
    heads,
    tokens_hbm,
    pre_hbm,
    w0,
    w1,
    w2,
    w3,
    w4,
    extra_hbm,
    bound_hbm,
    init_hbm,
    gain_hbm,
    out_ref,
    a4,
    a0,
    a1,
    a2,
    a3,
    tokens_ref,
    pre_ref,
    raw_ref,
    extra_ref,
    bound_ref,
    start_ref,
    init_ref,
    gain_ref,
    normed,
    f_v_ref,
    q_g_ref,
    cum_ref,
    keys_ref,
    rbuf,
    sbuf,
    send_sem,
    recv_sem,
    init_sem,
    y_send,
    y_recv,
    x_send,
    x_recv,
    s_send,
    s_recv,
    local_sem,
    e_send,
    e_recv,
):
    me = lax.axis_index("sp")
    rank = lax.axis_index("dp")
    items, hv, hk = rbuf.shape
    own = init_ref.shape[0]
    seqs, length, width = tokens_ref.shape
    cols = heads * hk
    tile = 2 * hk
    shards = (w0, w1, w2, w3, w4)
    wholes = (a0, a1, a2, a3, a4)
    side = lax.rem(me, 2)
    beside = me + 1 - 2 * side
    sibling = rank + 1 - 2 * lax.rem(rank, 2)
    peers = ways // 2 - 1

    def local_copy(w):
        return pltpu.make_async_copy(shards[w], full(w, rank), local_sem.at[w])

    def full(w, shard):
        rows = shards[w].shape[0]
        return wholes[w].at[pl.ds(pl.multiple_of(shard * rows, rows), rows)]

    small = [
        pltpu.make_async_copy(src, dst, local_sem.at[5 + j])
        for j, (src, dst) in enumerate(
            (
                (tokens_hbm, tokens_ref),
                (pre_hbm, pre_ref),
                (extra_hbm, raw_ref.at[me]),
                (bound_hbm, bound_ref),
                (init_hbm, start_ref),
                (gain_hbm, gain_ref),
            )
        )
    ]
    for w in range(5):
        local_copy(w).start()
    for copy in small:
        copy.start()

    barrier = pltpu.get_barrier_semaphore()
    for offset in range(1, n):
        pl.semaphore_signal(
            barrier, inc=1, device_id={"sp": lax.rem(me + offset, n)}, device_id_type=MESH
        )
    for offset in range(1, ways):
        pl.semaphore_signal(
            barrier, inc=1, device_id={"dp": lax.rem(rank + offset, ways)}, device_id_type=MESH
        )
    pl.semaphore_wait(barrier, n + ways - 2)

    def part(w, shard, half):
        rows = shards[w].shape[0]
        start = shard * rows + half * (rows // 2)
        return wholes[w].at[pl.ds(pl.multiple_of(start, rows // 2), rows // 2)]

    def remote(src, dst, send, recv, device):
        return pltpu.make_async_remote_copy(
            src_ref=src,
            dst_ref=dst,
            send_sem=send,
            recv_sem=recv,
            device_id=device,
            device_id_type=MESH,
        )

    def y_copy(w, k):
        ref = part(w, rank, side)
        target = lax.rem(rank + 2 * (k + 1), ways)
        return remote(ref, ref, y_send.at[w, k], y_recv.at[w, k], {"dp": target})

    def origin(k):
        return lax.rem(rank + ways - 2 * (k + 1), ways)

    def x_copy(w, k):
        ref = part(w, origin(k), side)
        return remote(ref, ref, x_send.at[w, k], x_recv.at[w, k], {"sp": beside})

    def s_own(w):
        ref = full(w, rank)
        return remote(ref, ref, s_send.at[w, 0], s_recv.at[w, 0], {"dp": sibling})

    def s_copy(w, k, second):
        ref = part(w, origin(k), 1 - side if second else side)
        slot = 1 + 2 * k + second
        return remote(ref, ref, s_send.at[w, slot], s_recv.at[w, slot], {"dp": sibling})

    def pass_y(w):
        for k in range(peers):
            y_copy(w, k).wait_recv()
            x_copy(w, k).start()
            s_copy(w, k, 0).start()

    def pass_x(w):
        for k in range(peers):
            x_copy(w, k).wait_recv()
            s_copy(w, k, 1).start()

    def arrived(w):
        s_own(w).wait_recv()
        for k in range(peers):
            s_copy(w, k, 0).wait_recv()
            s_copy(w, k, 1).wait_recv()

    def init_copy(j):
        return remote(
            init_ref.at[j],
            rbuf.at[me * own + j],
            init_sem.at[j],
            recv_sem.at[me * own + j],
            {"sp": 0},
        )

    def chain_copy(it):
        return remote(
            sbuf.at[it],
            rbuf.at[it],
            send_sem.at[it],
            recv_sem.at[it],
            {"sp": lax.rem(me + 1, n)},
        )

    def extra_copy(offset):
        return remote(
            raw_ref.at[me],
            raw_ref.at[me],
            e_send.at[offset - 1],
            e_recv.at[offset - 1],
            {"sp": lax.rem(me + offset, n)},
        )

    for w in range(5):
        local_copy(w).wait()
        for k in range(peers):
            y_copy(w, k).start()
        s_own(w).start()
    for copy in small:
        copy.wait()
    for offset in range(1, n):
        extra_copy(offset).start()
    for j in range(own):
        init_ref[j] = start_ref[j].T.astype(jnp.bfloat16)

    def norm_rows(s, carry):
        rows = pl.ds(pl.multiple_of(s * length, length), length)
        normed[rows, :] = rms_scale(tokens_ref[s], pre_ref[...]).astype(jnp.bfloat16)
        return carry

    lax.fori_loop(0, seqs, norm_rows, 0)

    @pl.when(me > 0)
    def _():
        for j in range(own):
            init_copy(j).start()

    @pl.when(me == 0)
    def _():
        rbuf[0:own] = init_ref[...]

    gap = 1.0 - bound_ref[...]
    row = lax.broadcasted_iota(jnp.int32, (length, length), 0)
    col = lax.broadcasted_iota(jnp.int32, (length, length), 1)
    causal = row >= col
    ones = causal.astype(jnp.float32)
    nt = (((1,), (1,)), ((), ()))
    tn = (((0,), (0,)), ((), ()))
    place = (length, n * length)
    chosen = (
        lax.broadcasted_iota(jnp.int32, place, 1)
        == lax.broadcasted_iota(jnp.int32, place, 0) + me * length
    ).astype(jnp.float32)
    for offset in range(1, n):
        extra_copy(offset).wait_recv()

    def pick(i, carry):
        extra_ref[i] = lax.dot_general(
            chosen,
            raw_ref[i],
            nt,
            precision=lax.Precision.HIGHEST,
            preferred_element_type=jnp.float32,
        )
        return carry

    lax.fori_loop(0, n, pick, 0)

    def project(w, dest, at, j):
        lanes = pl.ds(pl.multiple_of(j * tile, tile), tile)
        where = pl.ds(pl.multiple_of(at + j * tile, tile), tile)
        dest[:, where] = jnp.dot(
            normed[...], wholes[w][:, lanes], preferred_element_type=jnp.float32
        ).astype(jnp.bfloat16)

    def project_all(w, dest, at):
        def step(j, carry):
            project(w, dest, at, j)
            return carry

        lax.fori_loop(0, cols // tile, step, 0)

    pass_y(0)
    pass_y(1)
    pass_x(0)
    arrived(0)
    project_all(0, f_v_ref, 0)
    pass_x(1)
    pass_y(2)
    arrived(1)
    project_all(1, f_v_ref, cols)
    tiles = cols // tile

    def forward(s, carry):
        rows = pl.ds(pl.multiple_of(s * length, length), length)
        f_pre = f_v_ref[rows, 0:cols].astype(jnp.float32)
        keys = gap * jax.nn.sigmoid(-f_pre)
        spread = jnp.concatenate(
            [
                jnp.broadcast_to(
                    extra_ref[s * (heads // own) + h // own][:, h % own : h % own + 1],
                    (length, hk),
                )
                for h in range(heads)
            ],
            axis=1,
        )
        decay = jnp.log1p(-keys) + spread
        cum = jnp.dot(
            ones, decay, precision=lax.Precision.HIGHEST, preferred_element_type=jnp.float32
        )
        end = cum[length - 1 : length, :]
        mid = cum[length // 2 : length // 2 + 1, :]
        keys_end = (keys * jnp.exp(end - cum)).astype(jnp.bfloat16)
        keys_ref[rows, :] = (keys * jnp.exp(mid - cum)).astype(jnp.bfloat16)
        cum_ref[rows, :] = cum
        end_decay = jnp.exp(end)
        added = []
        for h in range(heads):
            lanes = slice(h * hk, (h + 1) * hk)
            values = f_v_ref[rows, cols + h * hv : cols + (h + 1) * hv]
            added.append(
                lax.dot_general(
                    values, keys_end[:, lanes], tn, preferred_element_type=jnp.float32
                )
            )
        for h in range(heads):
            lanes = slice(h * hk, (h + 1) * hk)
            it = s * heads + h

            @pl.when(jnp.logical_or(me > 0, it >= own))
            def _():
                chain_copy(it).wait_recv()

            @pl.when(me < n - 1)
            def _():
                state = rbuf[it].astype(jnp.float32)
                sbuf[it] = (state * end_decay[:, lanes] + added[h]).astype(jnp.bfloat16)
                chain_copy(it).start()

        @pl.when(s == 0)
        def _():
            pass_x(2)
            pass_y(3)

        @pl.when(s == tiles)
        def _():
            arrived(2)

        @pl.when(s == 2 * tiles - 1)
        def _():
            pass_x(3)
            pass_y(4)

        @pl.when(s == 2 * tiles)
        def _():
            arrived(3)

        @pl.when(s == 3 * tiles)
        def _():
            pass_x(4)

        @pl.when(jnp.logical_and(s >= tiles, s < 2 * tiles))
        def _():
            project(2, q_g_ref, 0, s - tiles)

        @pl.when(jnp.logical_and(s >= 2 * tiles, s < 3 * tiles))
        def _():
            project(3, q_g_ref, cols, s - 2 * tiles)

        return carry

    lax.fori_loop(0, seqs, forward, 0)

    def outputs(s, carry):
        rows = pl.ds(pl.multiple_of(s * length, length), length)
        cum = cum_ref[rows, :]
        mid = cum[length // 2 : length // 2 + 1, :]
        q_pre = q_g_ref[rows, 0:cols].astype(jnp.float32)
        queries = q_pre * jax.nn.sigmoid(q_pre)
        q_carry = (queries * jnp.exp(cum)).astype(jnp.bfloat16)
        q_mid = (queries * jnp.exp(cum - mid)).astype(jnp.bfloat16)
        for h in range(heads):
            lanes = slice(h * hk, (h + 1) * hk)
            it = s * heads + h
            values = f_v_ref[rows, cols + h * hv : cols + (h + 1) * hv]
            scores = lax.dot_general(
                q_mid[:, lanes], keys_ref[rows, lanes], nt, preferred_element_type=jnp.float32
            )
            scores = jnp.where(causal, scores, 0.0).astype(jnp.bfloat16)
            outs = jnp.dot(scores, values, preferred_element_type=jnp.float32) + lax.dot_general(
                q_carry[:, lanes], rbuf[it], nt, preferred_element_type=jnp.float32
            )
            scaled = rms_scale(outs, gain_ref[...]).astype(jnp.bfloat16).astype(jnp.float32)
            g_pre = q_g_ref[rows, cols + h * hv : cols + (h + 1) * hv].astype(jnp.float32)
            out_ref[rows, h * hv : (h + 1) * hv] = (
                scaled * (g_pre * jax.nn.sigmoid(g_pre))
            ).astype(jnp.bfloat16)
        return carry

    lax.fori_loop(0, seqs, outputs, 0)
    arrived(4)
    for offset in range(1, n):
        extra_copy(offset).wait_send()
    for w in range(5):
        s_own(w).wait_send()
        for k in range(peers):
            y_copy(w, k).wait_send()
            x_copy(w, k).wait_send()
            s_copy(w, k, 0).wait_send()
            s_copy(w, k, 1).wait_send()

    @pl.when(me > 0)
    def _():
        for j in range(own):
            init_copy(j).wait_send()

    @pl.when(me < n - 1)
    def _():
        def done(it, carry):
            chain_copy(it).wait_send()
            return carry

        lax.fori_loop(0, items, done, 0)


def layer(tokens, pre, weights, extra, bound, init, gain, n, ways):
    own, hk, hv = init.shape
    seqs, length, width = tokens.shape
    items = own * n
    heads = items // seqs
    rows = seqs * length
    peers = max(ways // 2 - 1, 1)
    vmem = pl.BlockSpec(memory_space=pltpu.VMEM)
    dma = pltpu.SemaphoreType.DMA

    def whole(w):
        return (w.shape[0] * ways, w.shape[1])

    return pl.pallas_call(
        functools.partial(layer_kernel, n, ways, heads),
        out_shape=[
            jax.ShapeDtypeStruct((rows, heads * hv), jnp.bfloat16),
            jax.ShapeDtypeStruct(whole(weights[4]), jnp.bfloat16),
        ],
        in_specs=[pl.BlockSpec(memory_space=pltpu.HBM)] * 11,
        out_specs=[vmem] * 2,
        scratch_shapes=[pltpu.VMEM(whole(w), jnp.bfloat16) for w in weights[:4]]
        + [
            pltpu.VMEM(tokens.shape, jnp.bfloat16),
            pltpu.VMEM(pre.shape, jnp.float32),
            pltpu.VMEM((n,) + extra.shape, jnp.float32),
            pltpu.VMEM((n, length, own), jnp.float32),
            pltpu.VMEM(bound.shape, jnp.float32),
            pltpu.VMEM(init.shape, jnp.float32),
            pltpu.VMEM((own, hv, hk), jnp.bfloat16),
            pltpu.VMEM(gain.shape, jnp.float32),
            pltpu.VMEM((rows, width), jnp.bfloat16),
            pltpu.VMEM((rows, heads * (hk + hv)), jnp.bfloat16),
            pltpu.VMEM((rows, heads * (hk + hv)), jnp.bfloat16),
            pltpu.VMEM((rows, heads * hk), jnp.float32),
            pltpu.VMEM((rows, heads * hk), jnp.bfloat16),
            pltpu.VMEM((items, hv, hk), jnp.bfloat16),
            pltpu.VMEM((items, hv, hk), jnp.bfloat16),
            dma((items,)),
            dma((items,)),
            dma((own,)),
            dma((5, peers)),
            dma((5, peers)),
            dma((5, peers)),
            dma((5, peers)),
            dma((5, 1 + 2 * peers)),
            dma((5, 1 + 2 * peers)),
            dma((11,)),
            dma((n - 1,)),
            dma((n - 1,)),
        ],
        compiler_params=pltpu.CompilerParams(
            collective_id=0, has_side_effects=True, vmem_limit_bytes=48 * 1024 * 1024
        ),
        cost_estimate=pl.CostEstimate(
            flops=6 * 10**9, bytes_accessed=2 * 10**7, transcendentals=10**6
        ),
    )(tokens, pre, *weights, extra, bound, init, gain)


def body(
    n,
    ways,
    tokens,
    pre_gain,
    w_query,
    w_forget,
    w_value,
    w_gate,
    lower_bound,
    extra_decay,
    initial_state,
    norm_gain,
    w_out,
    post_gain,
):
    seq_count, local_len, width = tokens.shape
    gated, w_o = layer(
        tokens,
        pre_gain[None, :],
        (w_forget, w_value, w_query, w_gate, w_out),
        extra_decay,
        lower_bound[None, :],
        initial_state,
        norm_gain[None, :],
        n,
        ways,
    )
    mixed = jnp.dot(gated, w_o, preferred_element_type=jnp.float32)
    return rms_scale(mixed, post_gain).astype(jnp.bfloat16).reshape(seq_count, local_len, width)


def solution(mesh):
    in_specs = (
        P("dp", "sp", None),
        P(),
        P("dp", None),
        P("dp", None),
        P("dp", None),
        P("dp", None),
        P(),
        P(("dp", "sp"), None),
        P(("dp", "sp"), None, None),
        P(),
        P("dp", None),
        P(),
    )
    out_specs = P("dp", "sp", None)
    return jax.shard_map(
        functools.partial(body, mesh.shape["sp"], mesh.shape["dp"]),
        mesh=mesh,
        in_specs=in_specs,
        out_specs=out_specs,
        check_vma=False,
    )
```
